32 devices in a mesh: ep: 8 (over z, y), tp: 4 (over x, core).
Axes of the slice: x: 2, y: 2, z: 4, core: 2. Of those that a mesh axis runs over, the one named last changes fastest.
Arguments:
- tokens: bfloat16 [24, 2048], P('ep'), may hold values from -6 to 6
- mixer_gain: float32 [2048], replicated, may hold values from 0.1 to 1.9
- query_weight: bfloat16 [2048, 2048], P('ep', 'tp'), may hold values from -0.125 to 0.125
- key_cache: bfloat16 [24, 1024, 4, 128], P('ep', None, 'tp'), may hold values from -6 to 6
- value_cache: bfloat16 [24, 1024, 4, 128], P('ep', None, 'tp'), may hold values from -6 to 6
- seq_lengths: int32 [24], P('ep'), may hold values from 1 to 1024, as said below
- head_offset: float32 [16], P('tp'), may hold values from -8.5 to -3.5
- output_weight: bfloat16 [2048, 2048], P('tp', 'ep'), may hold values from -0.5 to 0.5
- expert_gain: float32 [2048], replicated, may hold values from 0.1 to 1.9
- expert_ids: int32 [24, 2], P('ep'), may hold values from 0 to 7, as said below
- route_weight: float32 [24, 2], P('ep'), may hold values from 0.2 to 1
- gate_weight: bfloat16 [8, 2048, 1024], P('ep', None, 'tp'), may hold values from -0.125 to 0.125
- up_weight: bfloat16 [8, 2048, 1024], P('ep', None, 'tp'), may hold values from -0.125 to 0.125
- down_weight: bfloat16 [8, 1024, 2048], P('ep', 'tp'), may hold values from -0.1875 to 0.1875
Outputs:
- layer_out: bfloat16 [24, 2048], P('ep', 'tp')
The draws below stay inside these ranges and needn't reach their ends.
Inputs may be any that keep to these rules, and one draw needn't show every extreme that they name: `seq_lengths`: some sequence holds all 1024 positions. `expert_ids`: the 2 experts of a row are different and lie in one group of 4 consecutive expert numbers. Among the 3 rows of one index of ep no expert is named by more than 2 rows, and some expert by exactly 2.
All inputs are finite; a program needn't handle non-finite values.
Results may differ from the reference program's by a relative error of at most 0.012.
Values may be sent and summed in bfloat16 or wider, within the bound.
No kernel may reach another device: no remote copies, remote signals or barrier semaphores. Data moves between devices by JAX's collectives and lax.ppermute only.
A program may use at most 64 MiB of HBM per device.

```python
import jax
import jax.numpy as jnp
from jax import lax

D = 2048
HEADS = 16
KV_HEADS = 4
HD = 128
FF_E = 1024
EPG = 4
TOP = 2
CACHE = 1024
B_DEV = 3
B_TOT = 24
EXPERTS = 8
GROUPS = 2
CAP = 2
N_TP = 4


def draw_seq_lengths(key, part):
    first = jax.random.randint(jax.random.fold_in(key, 11), (B_TOT,), 1, CACHE + 1)
    second = jax.random.randint(jax.random.fold_in(key, 12), (B_TOT,), 1, CACHE + 1)
    chosen = jax.random.randint(jax.random.fold_in(key, 13), (), 0, B_TOT)
    lengths = jnp.minimum(first, second)
    lengths = jnp.where(jnp.arange(B_TOT) == chosen, CACHE, lengths)
    return lengths.astype(jnp.int32)


def draw_expert_ids(key, part):
    blocks = B_TOT // B_DEV
    group_keys = jax.random.split(jax.random.fold_in(key, 21), blocks)
    group_order = jax.vmap(lambda single: jax.random.permutation(single, GROUPS))(group_keys)
    sets = jnp.arange(B_DEV) // CAP
    groups = group_order[:, sets]
    leads = jax.random.randint(jax.random.fold_in(key, 22), (blocks, GROUPS), 0, EPG)[:, sets]
    other_keys = jax.random.split(jax.random.fold_in(key, 23), blocks * B_DEV)
    others = jax.vmap(lambda single: jax.random.permutation(single, EPG - 1))(other_keys)[:, :TOP - 1] + 1
    others = others.reshape(blocks, B_DEV, TOP - 1)
    inside = jnp.concatenate([leads[:, :, None], (leads[:, :, None] + others) % EPG], axis=2)
    numbers = groups[:, :, None] * EPG + inside
    return numbers.reshape(B_TOT, TOP).astype(jnp.int32)


def block_scale(rng, extent, cuts, smallest, largest):
    loudness, own = 1.0, jax.random.fold_in(rng, 6)
    for axis_at, shards_of in cuts:
        steps = jnp.exp(jax.random.uniform(jax.random.fold_in(own, axis_at), (shards_of,), jnp.float32, smallest / len(cuts), largest / len(cuts)))
        loudness = loudness * jnp.repeat(steps, extent[axis_at] // shards_of).reshape([-1 if axis == axis_at else 1 for axis in range(len(extent))])
    return loudness


def normal_values(key, shape, deviation, most, shards=(), kind=jnp.bfloat16):
    array = jax.random.normal(key, shape, jnp.float32) * deviation
    if len(shards) > 0:
        array = block_scale(key, shape, shards, -0.22, 0.18) * array
    return jnp.clip(array, min=-most, max=most).astype(kind)


def setup_inputs(seed: int = 0) -> dict:
    seeds = jax.random.split(jax.random.key(seed), 15)
    return {
        "tokens": normal_values(seeds[0], (B_TOT, D), 1.0, 6.0, ((0, 8),)),
        "mixer_gain": jnp.clip(1.0 + 0.18 * jax.random.normal(seeds[1], (D,), jnp.float32), 0.1, 1.9),
        "query_weight": normal_values(seeds[2], (D, HEADS * HD), D ** -0.5, 0.125, ((0, 8), (1, 4))),
        "key_cache": normal_values(seeds[3], (B_TOT, CACHE, KV_HEADS, HD), 1.0, 6.0, ((0, 8), (2, 4))),
        "value_cache": normal_values(seeds[4], (B_TOT, CACHE, KV_HEADS, HD), 1.0, 6.0, ((0, 8), (2, 4))),
        "seq_lengths": draw_seq_lengths(jax.random.fold_in(seeds[14], 71), 0),
        "head_offset": jnp.clip(-8.5 + 5.0 * jax.random.uniform(seeds[6], (HEADS,), jnp.float32) ** block_scale(seeds[6], (HEADS,), ((0, 4),), -0.2, 0.2), -8.5, -3.5),
        "output_weight": normal_values(seeds[7], (HEADS * HD, D), HD ** -0.5, 0.5, ((0, 4), (1, 8))),
        "expert_gain": jnp.clip(1.0 + 0.18 * jax.random.normal(seeds[8], (D,), jnp.float32), 0.1, 1.9),
        "expert_ids": draw_expert_ids(jax.random.fold_in(seeds[14], 71), 0),
        "route_weight": jnp.clip(0.2 + 0.8 * jax.random.uniform(seeds[10], (B_TOT, TOP), jnp.float32) ** block_scale(seeds[10], (B_TOT, TOP), ((0, 8),), -0.2, 0.2), 0.2, 1.0),
        "gate_weight": normal_values(seeds[11], (EXPERTS, D, FF_E), D ** -0.5, 0.125, ((0, 8), (2, 4))),
        "up_weight": normal_values(seeds[12], (EXPERTS, D, FF_E), D ** -0.5, 0.125, ((0, 8), (2, 4))),
        "down_weight": normal_values(seeds[13], (EXPERTS, FF_E, D), FF_E ** -0.5, 0.1875, ((0, 8), (1, 4))),
    }


def rms_norm(values, gain):
    wide = values.astype(jnp.float32)
    scale = lax.rsqrt(lax.optimization_barrier(jnp.mean(wide * wide, axis=-1, keepdims=True)) + 1e-06)
    return (wide * scale * gain).astype(jnp.bfloat16)

def reference(tokens, mixer_gain, query_weight, key_cache, value_cache, seq_lengths, head_offset, output_weight, expert_gain, expert_ids, route_weight, gate_weight, up_weight, down_weight):
    normed = rms_norm(tokens, mixer_gain)
    query = jnp.dot(normed, query_weight, preferred_element_type=jnp.float32).astype(jnp.bfloat16)
    per_group = HEADS // KV_HEADS
    scale = HD ** (-0.5)
    offset = head_offset.reshape(KV_HEADS, per_group, 1)

    def attend(args):
        query_row, keys, values, length = args
        grouped = query_row.reshape(KV_HEADS, per_group, HD).astype(jnp.float32)
        score = jnp.einsum('kgd,skd->kgs', grouped, keys.astype(jnp.float32)) * scale + offset
        valid = (jnp.arange(CACHE, dtype=jnp.int32) < length)[None, None, :]
        log_take = jax.nn.log_sigmoid(score)
        log_pass = jnp.where(valid, jax.nn.log_sigmoid(-score), 0.0)
        later = lax.cumsum(log_pass, axis=2, reverse=True) - log_pass
        weight = jnp.where(valid, jnp.exp(log_take + later), 0.0).astype(jnp.bfloat16)
        result = jnp.einsum('kgs,skd->kgd', weight.astype(jnp.float32), values.astype(jnp.float32))
        return result.reshape(HEADS * HD).astype(jnp.bfloat16)
    mixed = lax.map(attend, (query, key_cache, value_cache, seq_lengths))
    quarter_width = HEADS * HD // N_TP
    total = tokens.astype(jnp.float32)
    for quarter in range(N_TP):
        part = jnp.dot(mixed[:, quarter * quarter_width:(quarter + 1) * quarter_width], output_weight[quarter * quarter_width:(quarter + 1) * quarter_width], preferred_element_type=jnp.float32).astype(jnp.bfloat16)
        total = total + lax.optimization_barrier(part).astype(jnp.float32)
    resid = total.astype(jnp.bfloat16)
    normed2 = rms_norm(resid, expert_gain)
    flat_ids = expert_ids.reshape(-1).astype(jnp.int32)
    row_ids = (jnp.arange(B_TOT * TOP, dtype=jnp.int32) // TOP).astype(jnp.int32)
    unit_width = FF_E // N_TP

    def expert(args):
        number, row_index = args
        row = lax.dynamic_slice_in_dim(normed2, row_index, 1, 0)
        gate = jnp.dot(row, gate_weight[number], preferred_element_type=jnp.float32)
        upward = jnp.dot(row, up_weight[number], preferred_element_type=jnp.float32)
        hidden = (jax.nn.silu(gate) * upward).astype(jnp.bfloat16)
        downs = down_weight[number]
        summed = jnp.zeros((1, D), jnp.float32)
        for quarter in range(N_TP):
            part = jnp.dot(hidden[:, quarter * unit_width:(quarter + 1) * unit_width], downs[quarter * unit_width:(quarter + 1) * unit_width], preferred_element_type=jnp.float32).astype(jnp.bfloat16)
            summed = summed + lax.optimization_barrier(part).astype(jnp.float32)
        return summed.astype(jnp.bfloat16)[0]
    outputs = lax.map(expert, (flat_ids, row_ids))
    weighted = outputs.reshape(B_TOT, TOP, D).astype(jnp.float32) * route_weight[:, :, None]
    return (resid.astype(jnp.float32) + lax.optimization_barrier(jnp.sum(weighted, axis=1))).astype(jnp.bfloat16)
```

```python
import functools

import jax
import jax.numpy as jnp
from jax import lax
from jax.experimental import pallas as pl
from jax.experimental.pallas import tpu as pltpu
from jax.sharding import PartitionSpec as P

LANES = 128


def rms_norm(values, gain):
    wide = values.astype(jnp.float32)
    scale = lax.rsqrt(jnp.mean(wide * wide, axis=-1, keepdims=True) + 1e-06)
    return (wide * scale * gain).astype(jnp.bfloat16)


def attend_body(length_ref, offset_ref, part_ref, key_ref, value_ref, out_ref):
    batch, places, head_size = key_ref.shape
    heads = offset_ref.shape[1]
    rows = -(-batch * heads // 8) * 8
    query = jnp.sum(part_ref[...], axis=0).astype(jnp.bfloat16)
    scale = head_size ** (-0.5)
    scores, lengths, offsets = [], [], []
    for b in range(batch):
        one = jnp.concatenate(
            [query[b : b + 1, h * head_size : (h + 1) * head_size] for h in range(heads)], axis=0
        )
        scores.append(
            lax.dot_general(
                one, key_ref[b], (((1,), (1,)), ((), ())), preferred_element_type=jnp.float32
            )
        )
        lengths.append(jnp.full((heads, places), length_ref[b], jnp.int32))
        for h in range(heads):
            offsets.append(jnp.full((1, places), offset_ref[0, h], jnp.float32))
    extra = rows - batch * heads
    if extra:
        scores.append(jnp.zeros((extra, places), jnp.float32))
        lengths.append(jnp.zeros((extra, places), jnp.int32))
        offsets.append(jnp.zeros((extra, places), jnp.float32))
    score = jnp.concatenate(scores, axis=0) * scale + jnp.concatenate(offsets, axis=0)
    valid = lax.broadcasted_iota(jnp.int32, (rows, places), 1) < jnp.concatenate(lengths, axis=0)
    soft = jnp.log1p(jnp.exp(-jnp.abs(score)))
    log_take = jnp.minimum(score, 0.0) - soft
    log_pass = jnp.where(valid, jnp.minimum(-score, 0.0) - soft, 0.0)
    chunks = places // LANES
    stacked = jnp.concatenate(
        [log_pass[:, c * LANES : (c + 1) * LANES] for c in range(chunks)], axis=0
    )
    high = stacked.astype(jnp.bfloat16)
    rest = stacked - high.astype(jnp.float32)
    middle = rest.astype(jnp.bfloat16)
    low = (rest - middle.astype(jnp.float32)).astype(jnp.bfloat16)
    source = lax.broadcasted_iota(jnp.int32, (LANES, LANES), 0)
    target = lax.broadcasted_iota(jnp.int32, (LANES, LANES), 1)
    after = (source > target).astype(jnp.bfloat16)
    dot = functools.partial(jnp.dot, preferred_element_type=jnp.float32)
    inside = dot(low, after) + dot(middle, after) + dot(high, after)
    totals = jnp.sum(stacked, axis=1, keepdims=True)
    later = jnp.zeros((rows, 1), jnp.float32)
    pieces = [None] * chunks
    for c in reversed(range(chunks)):
        pieces[c] = inside[c * rows : (c + 1) * rows] + later
        later = later + totals[c * rows : (c + 1) * rows]
    weight = jnp.where(valid, jnp.exp(log_take + jnp.concatenate(pieces, axis=1)), 0.0)
    weight = weight.astype(jnp.bfloat16)
    for b in range(batch):
        mixed = dot(weight, value_ref[b]).astype(jnp.bfloat16)
        for h in range(heads):
            out_ref[b : b + 1, h * head_size : (h + 1) * head_size] = mixed[
                b * heads + h : b * heads + h + 1
            ]


def attend(parts, keys, values, lengths, offset):
    batch, _, head_size = keys.shape
    width = parts.shape[2]
    vmem = pl.BlockSpec(memory_space=pltpu.VMEM)
    smem = pl.BlockSpec(memory_space=pltpu.SMEM)
    return pl.pallas_call(
        attend_body,
        out_shape=jax.ShapeDtypeStruct((batch, width), jnp.bfloat16),
        in_specs=[smem, smem, vmem, vmem, vmem],
        out_specs=vmem,
        name="attend",
    )(lengths, offset.reshape(1, -1), parts, keys, values)


def spread(block, axes, count):
    wide = jnp.broadcast_to(block[None], (count,) + block.shape)
    return lax.all_to_all(wide, axes, split_axis=0, concat_axis=0, tiled=True)


def local(
    tokens,
    mixer_gain,
    query_weight,
    key_cache,
    value_cache,
    seq_lengths,
    head_offset,
    output_weight,
    expert_gain,
    expert_ids,
    route_weight,
    gate_weight,
    up_weight,
    down_weight,
):
    ep_count = lax.axis_size("ep")
    tp_count = lax.axis_size("tp")
    ep_index = lax.axis_index("ep")
    tp_index = lax.axis_index("tp")
    batch, width = tokens.shape
    total = ep_count * batch
    both = ("ep", "tp")
    columns = output_weight.shape[1]
    out_weight = lax.all_gather(output_weight, "tp", axis=0)

    all_tokens = spread(tokens, "ep", ep_count).reshape(total, width)
    normed = rms_norm(all_tokens, mixer_gain)
    feature_count = query_weight.shape[0]
    features = lax.dynamic_slice_in_dim(normed, ep_index * feature_count, feature_count, 1)
    partial_query = jnp.dot(features, query_weight, preferred_element_type=jnp.float32)
    parts = lax.all_to_all(partial_query, "ep", split_axis=0, concat_axis=0, tiled=True)
    parts = parts.reshape(ep_count, batch, parts.shape[1])

    batch_places = key_cache.shape[:2]
    keys = key_cache.reshape(*batch_places, -1)
    values = value_cache.reshape(*batch_places, -1)
    mixed = attend(parts, keys, values, seq_lengths, head_offset)

    spread_mixed = spread(mixed, both, ep_count * tp_count)
    spread_mixed = spread_mixed.reshape(ep_count, tp_count, batch, -1)
    token_columns = lax.dynamic_slice_in_dim(all_tokens, ep_index * columns, columns, 1)
    summed = token_columns.astype(jnp.float32)
    for quarter in range(tp_count):
        rows = spread_mixed[:, quarter].reshape(total, -1)
        part = jnp.dot(rows, out_weight[quarter], preferred_element_type=jnp.float32)
        summed = summed + part.astype(jnp.bfloat16).astype(jnp.float32)
    resid_columns = summed.astype(jnp.bfloat16)
    resid = spread(resid_columns, "ep", ep_count)
    resid = resid.reshape(ep_count, total, columns).transpose(1, 0, 2).reshape(total, width)

    normed2 = rms_norm(resid, expert_gain)
    gate = jnp.dot(normed2, gate_weight[0], preferred_element_type=jnp.float32)
    upward = jnp.dot(normed2, up_weight[0], preferred_element_type=jnp.float32)
    hidden = (jax.nn.silu(gate) * upward).astype(jnp.bfloat16)
    term = jnp.dot(hidden, down_weight[0], preferred_element_type=jnp.float32).astype(jnp.bfloat16)
    slice_width = width // tp_count
    outgoing = term.reshape(ep_count, batch, tp_count, slice_width).transpose(0, 2, 1, 3)
    outgoing = outgoing.reshape(ep_count * tp_count, batch, slice_width)
    returned = lax.all_to_all(outgoing, both, split_axis=0, concat_axis=0, tiled=True)
    returned = returned.reshape(ep_count, tp_count, batch, slice_width)
    expert_out = jnp.sum(returned.astype(jnp.float32), axis=1).astype(jnp.bfloat16)
    numbers = jnp.arange(ep_count, dtype=jnp.int32)[:, None, None]
    share = jnp.sum(jnp.where(expert_ids[None] == numbers, route_weight[None], 0.0), axis=2)
    mixture = jnp.sum(expert_out.astype(jnp.float32) * share[:, :, None], axis=0)
    own = lax.dynamic_slice(
        resid, (ep_index * batch, tp_index * slice_width), (batch, slice_width)
    )
    return (own.astype(jnp.float32) + mixture).astype(jnp.bfloat16)


def solution(mesh):
    in_specs = (
        P("ep", None),
        P(),
        P("ep", "tp"),
        P("ep", None, "tp", None),
        P("ep", None, "tp", None),
        P("ep"),
        P("tp"),
        P("tp", "ep"),
        P(),
        P("ep", None),
        P("ep", None),
        P("ep", None, "tp"),
        P("ep", None, "tp"),
        P("ep", "tp", None),
    )
    out_specs = P("ep", "tp")
    return jax.shard_map(local, mesh=mesh, in_specs=in_specs, out_specs=out_specs, check_vma=False)
```

```python
import functools

import jax
import jax.numpy as jnp
from jax import lax
from jax.experimental import pallas as pl
from jax.experimental.pallas import tpu as pltpu
from jax.sharding import PartitionSpec as P

LANES = 128


def rms_norm(values, gain):
    wide = values.astype(jnp.float32)
    scale = lax.rsqrt(jnp.mean(wide * wide, axis=-1, keepdims=True) + 1e-06)
    return (wide * scale * gain).astype(jnp.bfloat16)


def attend_body(length_ref, offset_ref, part_ref, token_ref, key_ref, value_ref, out_ref):
    batch, places, head_size = key_ref.shape
    heads = offset_ref.shape[1]
    rows = -(-batch * heads // 8) * 8
    wide = token_ref[...].astype(jnp.float32)
    norm = lax.rsqrt(jnp.mean(wide * wide, axis=-1, keepdims=True) + 1e-06)
    query = (jnp.sum(part_ref[...], axis=0) * norm).astype(jnp.bfloat16)
    scale = head_size ** (-0.5)
    scores, lengths, offsets = [], [], []
    for b in range(batch):
        one = jnp.concatenate(
            [query[b : b + 1, h * head_size : (h + 1) * head_size] for h in range(heads)], axis=0
        )
        scores.append(
            lax.dot_general(
                one, key_ref[b], (((1,), (1,)), ((), ())), preferred_element_type=jnp.float32
            )
        )
        lengths.append(jnp.full((heads, places), length_ref[b], jnp.int32))
        for h in range(heads):
            offsets.append(jnp.full((1, places), offset_ref[0, h], jnp.float32))
    extra = rows - batch * heads
    if extra:
        scores.append(jnp.zeros((extra, places), jnp.float32))
        lengths.append(jnp.zeros((extra, places), jnp.int32))
        offsets.append(jnp.zeros((extra, places), jnp.float32))
    score = jnp.concatenate(scores, axis=0) * scale + jnp.concatenate(offsets, axis=0)
    valid = lax.broadcasted_iota(jnp.int32, (rows, places), 1) < jnp.concatenate(lengths, axis=0)
    soft = jnp.log1p(jnp.exp(-jnp.abs(score)))
    log_take = jnp.minimum(score, 0.0) - soft
    log_pass = jnp.where(valid, jnp.minimum(-score, 0.0) - soft, 0.0)
    chunks = places // LANES
    stacked = jnp.concatenate(
        [log_pass[:, c * LANES : (c + 1) * LANES] for c in range(chunks)], axis=0
    )
    high = stacked.astype(jnp.bfloat16)
    rest = stacked - high.astype(jnp.float32)
    middle = rest.astype(jnp.bfloat16)
    low = (rest - middle.astype(jnp.float32)).astype(jnp.bfloat16)
    source = lax.broadcasted_iota(jnp.int32, (LANES, LANES), 0)
    target = lax.broadcasted_iota(jnp.int32, (LANES, LANES), 1)
    after = (source > target).astype(jnp.bfloat16)
    dot = functools.partial(jnp.dot, preferred_element_type=jnp.float32)
    inside = dot(low, after) + dot(middle, after) + dot(high, after)
    totals = jnp.sum(stacked, axis=1, keepdims=True)
    later = jnp.zeros((rows, 1), jnp.float32)
    pieces = [None] * chunks
    for c in reversed(range(chunks)):
        pieces[c] = inside[c * rows : (c + 1) * rows] + later
        later = later + totals[c * rows : (c + 1) * rows]
    weight = jnp.where(valid, jnp.exp(log_take + jnp.concatenate(pieces, axis=1)), 0.0)
    weight = weight.astype(jnp.bfloat16)
    mixed_rows = []
    for b in range(batch):
        mixed = dot(weight, value_ref[b])
        mixed_rows.append(
            jnp.concatenate([mixed[b * heads + h : b * heads + h + 1] for h in range(heads)], axis=1)
        )
    mixed = jnp.concatenate(mixed_rows, axis=0).astype(jnp.bfloat16)
    for copy in range(out_ref.shape[0]):
        out_ref[copy] = mixed


def attend(parts, tokens, keys, values, lengths, offset, copies):
    batch = tokens.shape[0]
    vmem = pl.BlockSpec(memory_space=pltpu.VMEM)
    smem = pl.BlockSpec(memory_space=pltpu.SMEM)
    return pl.pallas_call(
        attend_body,
        out_shape=jax.ShapeDtypeStruct((copies, batch, parts.shape[2]), jnp.bfloat16),
        in_specs=[smem, smem, vmem, vmem, vmem, vmem],
        out_specs=vmem,
        name="attend",
    )(lengths, offset.reshape(1, -1), parts, tokens, keys, values)


def spread(block, axes, count):
    wide = jnp.broadcast_to(block[None], (count,) + block.shape)
    return lax.all_to_all(wide, axes, split_axis=0, concat_axis=0, tiled=True)


def local(
    tokens,
    mixer_gain,
    query_weight,
    key_cache,
    value_cache,
    seq_lengths,
    head_offset,
    output_weight,
    expert_gain,
    expert_ids,
    route_weight,
    gate_weight,
    up_weight,
    down_weight,
):
    ep_count = lax.axis_size("ep")
    tp_count = lax.axis_size("tp")
    ep_index = lax.axis_index("ep")
    tp_index = lax.axis_index("tp")
    batch, width = tokens.shape
    total = ep_count * batch
    both = ("ep", "tp")
    columns = output_weight.shape[1]

    feature_count = query_weight.shape[0]
    raw = lax.all_to_all(tokens, "ep", split_axis=1, concat_axis=0, tiled=True)
    gain = lax.dynamic_slice_in_dim(mixer_gain, ep_index * feature_count, feature_count, 0)
    features = (raw.astype(jnp.float32) * gain).astype(jnp.bfloat16)
    partial_query = jnp.dot(features, query_weight, preferred_element_type=jnp.float32)
    parts = lax.all_to_all(partial_query, "ep", split_axis=0, concat_axis=0, tiled=True)
    parts = parts.reshape(ep_count, batch, parts.shape[1])

    batch_places = key_cache.shape[:2]
    keys = key_cache.reshape(*batch_places, -1)
    values = value_cache.reshape(*batch_places, -1)
    outward = attend(parts, tokens, keys, values, seq_lengths, head_offset, ep_count)
    inward = lax.all_to_all(outward, "ep", split_axis=0, concat_axis=0, tiled=True)
    heads_out = inward.reshape(total, -1)
    part = jnp.dot(heads_out, output_weight, preferred_element_type=jnp.float32)
    part = part + jnp.where(tp_index == 0, raw.astype(jnp.float32), 0.0)
    terms = spread(part.astype(jnp.bfloat16), both, ep_count * tp_count)
    terms = terms.reshape(ep_count, tp_count, total, columns)
    resid = jnp.sum(terms.astype(jnp.float32), axis=1).astype(jnp.bfloat16)
    resid = resid.transpose(1, 0, 2).reshape(total, width)

    normed2 = rms_norm(resid, expert_gain)
    gate = jnp.dot(normed2, gate_weight[0], preferred_element_type=jnp.float32)
    upward = jnp.dot(normed2, up_weight[0], preferred_element_type=jnp.float32)
    hidden = (jax.nn.silu(gate) * upward).astype(jnp.bfloat16)
    term = jnp.dot(hidden, down_weight[0], preferred_element_type=jnp.float32).astype(jnp.bfloat16)
    slice_width = width // tp_count
    outgoing = term.reshape(ep_count, batch, tp_count, slice_width).transpose(0, 2, 1, 3)
    outgoing = outgoing.reshape(ep_count * tp_count, batch, slice_width)
    returned = lax.all_to_all(outgoing, both, split_axis=0, concat_axis=0, tiled=True)
    returned = returned.reshape(ep_count, tp_count, batch, slice_width)
    expert_out = jnp.sum(returned.astype(jnp.float32), axis=1).astype(jnp.bfloat16)
    numbers = jnp.arange(ep_count, dtype=jnp.int32)[:, None, None]
    share = jnp.sum(jnp.where(expert_ids[None] == numbers, route_weight[None], 0.0), axis=2)
    mixture = jnp.sum(expert_out.astype(jnp.float32) * share[:, :, None], axis=0)
    own = lax.dynamic_slice(
        resid, (ep_index * batch, tp_index * slice_width), (batch, slice_width)
    )
    return (own.astype(jnp.float32) + mixture).astype(jnp.bfloat16)


def solution(mesh):
    in_specs = (
        P("ep", None),
        P(),
        P("ep", "tp"),
        P("ep", None, "tp", None),
        P("ep", None, "tp", None),
        P("ep"),
        P("tp"),
        P("tp", "ep"),
        P(),
        P("ep", None),
        P("ep", None),
        P("ep", None, "tp"),
        P("ep", None, "tp"),
        P("ep", "tp", None),
    )
    out_specs = P("ep", "tp")
    return jax.shard_map(local, mesh=mesh, in_specs=in_specs, out_specs=out_specs, check_vma=False)
```

```python
import functools

import jax
import jax.numpy as jnp
from jax import lax
from jax.experimental import pallas as pl
from jax.experimental.pallas import tpu as pltpu
from jax.sharding import PartitionSpec as P

LANES = 128


def rms_norm(values, gain):
    wide = values.astype(jnp.float32)
    scale = lax.rsqrt(jnp.mean(wide * wide, axis=-1, keepdims=True) + 1e-06)
    return (wide * scale * gain).astype(jnp.bfloat16)


def attend_body(length_ref, offset_ref, part_ref, token_ref, key_ref, value_ref, out_ref):
    batch, places, head_size = key_ref.shape
    heads = offset_ref.shape[0]
    rows = -(-batch * heads // 8) * 8
    wide = token_ref[...].astype(jnp.float32)
    norm = lax.rsqrt(jnp.mean(wide * wide, axis=-1, keepdims=True) + 1e-06)
    query = (jnp.sum(part_ref[...], axis=0) * norm).astype(jnp.bfloat16)
    scale = head_size ** (-0.5)
    scores, lengths, offsets = [], [], []
    for b in range(batch):
        one = jnp.concatenate(
            [query[b : b + 1, h * head_size : (h + 1) * head_size] for h in range(heads)], axis=0
        )
        scores.append(
            lax.dot_general(
                one, key_ref[b], (((1,), (1,)), ((), ())), preferred_element_type=jnp.float32
            )
        )
        lengths.append(jnp.full((heads, places), length_ref[b], jnp.int32))
        for h in range(heads):
            offsets.append(jnp.full((1, places), offset_ref[h], jnp.float32))
    extra = rows - batch * heads
    if extra:
        scores.append(jnp.zeros((extra, places), jnp.float32))
        lengths.append(jnp.zeros((extra, places), jnp.int32))
        offsets.append(jnp.zeros((extra, places), jnp.float32))
    score = jnp.concatenate(scores, axis=0) * scale + jnp.concatenate(offsets, axis=0)
    valid = lax.broadcasted_iota(jnp.int32, (rows, places), 1) < jnp.concatenate(lengths, axis=0)
    soft = jnp.log1p(jnp.exp(-jnp.abs(score)))
    log_take = jnp.minimum(score, 0.0) - soft
    log_pass = jnp.where(valid, jnp.minimum(-score, 0.0) - soft, 0.0)
    chunks = places // LANES
    stacked = jnp.concatenate(
        [log_pass[:, c * LANES : (c + 1) * LANES] for c in range(chunks)], axis=0
    )
    high = stacked.astype(jnp.bfloat16)
    rest = stacked - high.astype(jnp.float32)
    middle = rest.astype(jnp.bfloat16)
    low = (rest - middle.astype(jnp.float32)).astype(jnp.bfloat16)
    source = lax.broadcasted_iota(jnp.int32, (LANES, LANES), 0)
    target = lax.broadcasted_iota(jnp.int32, (LANES, LANES), 1)
    after = (source > target).astype(jnp.bfloat16)
    dot = functools.partial(jnp.dot, preferred_element_type=jnp.float32)
    inside = dot(low, after) + dot(middle, after) + dot(high, after)
    totals = jnp.sum(stacked, axis=1, keepdims=True)
    later = jnp.zeros((rows, 1), jnp.float32)
    pieces = [None] * chunks
    for c in reversed(range(chunks)):
        pieces[c] = inside[c * rows : (c + 1) * rows] + later
        later = later + totals[c * rows : (c + 1) * rows]
    weight = jnp.where(valid, jnp.exp(log_take + jnp.concatenate(pieces, axis=1)), 0.0)
    weight = weight.astype(jnp.bfloat16)
    mixed_rows = []
    for b in range(batch):
        mixed = dot(weight, value_ref[b])
        mixed_rows.append(
            jnp.concatenate([mixed[b * heads + h : b * heads + h + 1] for h in range(heads)], axis=1)
        )
    mixed = jnp.concatenate(mixed_rows, axis=0).astype(jnp.bfloat16)
    for copy in range(out_ref.shape[0]):
        out_ref[copy] = mixed


def attend(parts, tokens, keys, values, lengths, offset, copies):
    batch = tokens.shape[0]
    vmem = pl.BlockSpec(memory_space=pltpu.VMEM)
    smem = pl.BlockSpec(memory_space=pltpu.SMEM)
    return pl.pallas_call(
        attend_body,
        out_shape=jax.ShapeDtypeStruct((copies, batch, parts.shape[2]), jnp.bfloat16),
        in_specs=[smem, smem, vmem, vmem, vmem, vmem],
        out_specs=vmem,
        name="attend",
    )(lengths, offset, parts, tokens, keys, values)


def spread(block, axes, count):
    wide = jnp.broadcast_to(block[None], (count,) + block.shape)
    return lax.all_to_all(wide, axes, split_axis=0, concat_axis=0, tiled=True)


def local(
    tokens,
    mixer_gain,
    query_weight,
    key_cache,
    value_cache,
    seq_lengths,
    head_offset,
    output_weight,
    expert_gain,
    expert_ids,
    route_weight,
    gate_weight,
    up_weight,
    down_weight,
):
    ep_count = lax.axis_size("ep")
    tp_count = lax.axis_size("tp")
    ep_index = lax.axis_index("ep")
    tp_index = lax.axis_index("tp")
    batch, width = tokens.shape
    total = ep_count * batch
    both = ("ep", "tp")
    columns = output_weight.shape[1]

    out_weights = [output_weight] + [
        lax.ppermute(output_weight, "tp", [(s, s ^ step) for s in range(tp_count)])
        for step in range(1, tp_count)
    ]
    feature_count = query_weight.shape[0]
    raw = lax.all_to_all(tokens, "ep", split_axis=1, concat_axis=0, tiled=True)
    gain = lax.dynamic_slice_in_dim(mixer_gain, ep_index * feature_count, feature_count, 0)
    features = (raw.astype(jnp.float32) * gain).astype(jnp.bfloat16)
    partial_query = jnp.dot(features, query_weight, preferred_element_type=jnp.float32)
    parts = lax.all_to_all(partial_query, "ep", split_axis=0, concat_axis=0, tiled=True)
    parts = parts.reshape(ep_count, batch, parts.shape[1])

    batch_places = key_cache.shape[:2]
    keys = key_cache.reshape(*batch_places, -1)
    values = value_cache.reshape(*batch_places, -1)
    outward = attend(parts, tokens, keys, values, seq_lengths, head_offset, ep_count * tp_count)
    inward = lax.all_to_all(outward, both, split_axis=0, concat_axis=0, tiled=True)
    inward = inward.reshape(ep_count, tp_count, batch, -1)
    summed = raw.astype(jnp.float32)
    for step in range(tp_count):
        quarter = lax.dynamic_index_in_dim(inward, tp_index ^ step, 1, keepdims=False)
        part = jnp.dot(
            quarter.reshape(total, -1), out_weights[step], preferred_element_type=jnp.float32
        )
        summed = summed + part.astype(jnp.bfloat16).astype(jnp.float32)
    resid = spread(summed.astype(jnp.bfloat16), "ep", ep_count)
    resid = resid.transpose(1, 0, 2).reshape(total, width)

    normed2 = rms_norm(resid, expert_gain)
    gate = jnp.dot(normed2, gate_weight[0], preferred_element_type=jnp.float32)
    upward = jnp.dot(normed2, up_weight[0], preferred_element_type=jnp.float32)
    hidden = (jax.nn.silu(gate) * upward).astype(jnp.bfloat16)
    term = jnp.dot(hidden, down_weight[0], preferred_element_type=jnp.float32).astype(jnp.bfloat16)
    slice_width = width // tp_count
    outgoing = term.reshape(ep_count, batch, tp_count, slice_width).transpose(0, 2, 1, 3)
    outgoing = outgoing.reshape(ep_count * tp_count, batch, slice_width)
    returned = lax.all_to_all(outgoing, both, split_axis=0, concat_axis=0, tiled=True)
    returned = returned.reshape(ep_count, tp_count, batch, slice_width)
    expert_out = jnp.sum(returned.astype(jnp.float32), axis=1).astype(jnp.bfloat16)
    numbers = jnp.arange(ep_count, dtype=jnp.int32)[:, None, None]
    share = jnp.sum(jnp.where(expert_ids[None] == numbers, route_weight[None], 0.0), axis=2)
    mixture = jnp.sum(expert_out.astype(jnp.float32) * share[:, :, None], axis=0)
    own = lax.dynamic_slice(
        resid, (ep_index * batch, tp_index * slice_width), (batch, slice_width)
    )
    return (own.astype(jnp.float32) + mixture).astype(jnp.bfloat16)


def solution(mesh):
    in_specs = (
        P("ep", None),
        P(),
        P("ep", "tp"),
        P("ep", None, "tp", None),
        P("ep", None, "tp", None),
        P("ep"),
        P("tp"),
        P("tp", "ep"),
        P(),
        P("ep", None),
        P("ep", None),
        P("ep", None, "tp"),
        P("ep", None, "tp"),
        P("ep", "tp", None),
    )
    out_specs = P("ep", "tp")
    return jax.shard_map(local, mesh=mesh, in_specs=in_specs, out_specs=out_specs, check_vma=False)
```
